32 devices in a mesh: fs: 8 (over z, x), tp: 4 (over y, core).
Axes of the slice: x: 2, y: 2, z: 4, core: 2. Of those that a mesh axis runs over, the one named last changes fastest.
Arguments:
- tokens: bfloat16 [3584, 2304], P('fs'), may hold values from -6 to 6
- norm_gain: float32 [2304], replicated, may hold values from 0.1 to 1.9
- gate_weight: bfloat16 [2304, 6144], P('fs', 'tp'), may hold values from -0.125 to 0.125
- up_weight: bfloat16 [2304, 6144], P('fs', 'tp'), may hold values from -0.125 to 0.125
- down_weight: bfloat16 [6144, 2304], P('tp', 'fs'), may hold values from -0.078125 to 0.078125
- branch_gain: float32 [2304], replicated, may hold values from 0.1 to 1.9
Outputs:
- result: bfloat16 [3584, 2304], P('fs')
The draws below stay inside these ranges and needn't reach their ends.
All inputs are finite; a program needn't handle non-finite values.
Results may differ from the reference program's by a relative error of at most 0.014.
Values may be sent and summed in bfloat16 or wider, within the bound.
A program may use at most 64 MiB of HBM per device.

```python
import jax
import jax.numpy as jnp
from jax import lax

D = 2304
FF = 6144
TOKENS = 3584
N_TP = 4


def shard_levels(own_key, dims, split, smallest, high):
    level, own = 1.0, jax.random.fold_in(own_key, 6)
    for position, blocks in split:
        draws = jnp.exp(jax.random.uniform(jax.random.fold_in(own, position), (blocks,), jnp.float32, smallest / len(split), high / len(split)))
        level = level * jnp.repeat(draws, dims[position] // blocks).reshape([-1 if axis == position else 1 for axis in range(len(dims))])
    return level


def scatter_about(rng, shape, spread, bound, split=(), held_as=jnp.bfloat16):
    entries = jax.random.normal(rng, shape, jnp.float32) * spread
    if len(split) > 0:
        entries = shard_levels(rng, shape, split, -0.22, 0.18) * entries
    return jnp.clip(entries, min=-bound, max=bound).astype(held_as)


def setup_inputs(seed: int = 0) -> dict:
    key_of = jax.random.split(jax.random.key(seed), 7)
    tokens = scatter_about(key_of[0], (TOKENS, D), 1.0, 6.0, ((0, 8),))
    norm_gain = jnp.clip(1.0 + 0.18 * jax.random.normal(key_of[1], (D,), jnp.float32), 0.1, 1.9)
    gate_weight = scatter_about(key_of[2], (D, FF), D ** -0.5, 0.125, ((0, 8), (1, 4)))
    up_weight = scatter_about(key_of[3], (D, FF), D ** -0.5, 0.125, ((0, 8), (1, 4)))
    down_weight = scatter_about(key_of[4], (FF, D), FF ** -0.5, 0.078125, ((0, 4), (1, 8)))
    branch_gain = jnp.clip(1.0 + 0.18 * jax.random.normal(key_of[5], (D,), jnp.float32), 0.1, 1.9)
    return {"tokens": tokens, "norm_gain": norm_gain, "gate_weight": gate_weight, "up_weight": up_weight, "down_weight": down_weight, "branch_gain": branch_gain}


epsilon = 1e-06

def reference(tokens, norm_gain, gate_weight, up_weight, down_weight, branch_gain):
    widened = tokens.astype(jnp.float32)
    scale = lax.rsqrt(lax.optimization_barrier(jnp.mean(widened * widened, axis=-1, keepdims=True)) + epsilon)
    normed = (widened * scale * norm_gain).astype(jnp.bfloat16)
    width = FF // N_TP
    branch = jnp.zeros(tokens.shape, jnp.float32)
    for block_index in range(N_TP):
        begin = block_index * width
        gate_sum = jnp.dot(normed, gate_weight[:, begin:begin + width], preferred_element_type=jnp.float32)
        up_sum = jnp.dot(normed, up_weight[:, begin:begin + width], preferred_element_type=jnp.float32)
        hidden = (jax.nn.silu(gate_sum) * up_sum).astype(jnp.bfloat16)
        partial_value = jnp.dot(hidden, down_weight[begin:begin + width, :], preferred_element_type=jnp.float32)
        branch = branch + partial_value.astype(jnp.bfloat16).astype(jnp.float32)
    branch_scale = lax.rsqrt(lax.optimization_barrier(jnp.mean(branch * branch, axis=-1, keepdims=True)) + epsilon)
    return (widened + branch * branch_scale * branch_gain).astype(jnp.bfloat16)
```

```python
import functools

import jax
import jax.numpy as jnp
from jax import lax
from jax.experimental import pallas as pl
from jax.experimental.pallas import tpu as pltpu
from jax.sharding import PartitionSpec as P

MESH = pl.DeviceIdType.MESH
epsilon = 1e-06
SUB = 3


def complete(own_tokens, summed, branch_gain):
    branch_scale = lax.rsqrt(jnp.mean(summed * summed, axis=-1, keepdims=True) + epsilon)
    return (own_tokens.astype(jnp.float32) + summed * branch_scale * branch_gain).astype(
        jnp.bfloat16
    )


def normalize(tokens, norm_gain):
    widened = tokens.astype(jnp.float32)
    scale = lax.rsqrt(jnp.mean(widened * widened, axis=-1, keepdims=True) + epsilon)
    return (widened * scale * norm_gain).astype(jnp.bfloat16)


def plain(tokens, norm_gain, gate_weight, up_weight, down_weight, branch_gain):
    normed = normalize(tokens, norm_gain)
    gate_whole, up_whole = (
        lax.all_gather(gate_weight, "fs", axis=0, tiled=True),
        lax.all_gather(up_weight, "fs", axis=0, tiled=True),
    )
    gate_sum = jnp.dot(normed, gate_whole, preferred_element_type=jnp.float32)
    up_sum = jnp.dot(normed, up_whole, preferred_element_type=jnp.float32)
    hidden = (jax.nn.silu(gate_sum) * up_sum).astype(jnp.bfloat16)
    partial_value = jnp.dot(
        hidden,
        lax.all_gather(down_weight, "fs", axis=1, tiled=True),
        preferred_element_type=jnp.float32,
    )
    summed = lax.psum(partial_value.astype(jnp.bfloat16), "tp").astype(jnp.float32)
    return complete(tokens, summed, branch_gain)


def log2(n):
    return n.bit_length() - 1


def kernel(n_fs, n_tp, group, tokens_ref, normed_ref, gate_ref, up_ref, down_ref, gain_ref, out_ref, *scratch):
    n_group = n_fs // group
    stages = log2(group * n_tp)
    tp_bits = log2(n_tp)
    xs, wg, wu, wd, hid, own, fin = scratch[:7]
    held = scratch[7:7 + stages]
    arrived = scratch[7 + stages:7 + 2 * stages]
    (loc_sem, w_send, w_recv, x_send, x_recv, y_send, y_recv, r_send, r_recv, o_send, o_recv) = scratch[7 + 2 * stages:]
    f, t = lax.axis_index("fs"), lax.axis_index("tp")
    g, q = f // group, f % group
    rank = q * n_tp + t
    depth, width = gate_ref.shape[0], wg.shape[1]
    chunks, rq, cw = fin.shape
    rows = n_tp * rq

    barrier = pltpu.get_barrier_semaphore()
    for k in range(1, n_fs):
        pl.semaphore_signal(barrier, inc=1, device_id=((f + k) % n_fs, t), device_id_type=MESH)
    for k in range(1, n_tp):
        pl.semaphore_signal(barrier, inc=1, device_id=(f, (t + k) % n_tp), device_id_type=MESH)

    at = pl.ds(pl.multiple_of(f * depth, depth), depth)
    mine = pl.ds(pl.multiple_of(q * width, width), width)
    local = [
        pltpu.make_async_copy(normed_ref, xs.at[q], loc_sem.at[0]),
        pltpu.make_async_copy(gate_ref.at[:, mine], wg.at[at], loc_sem.at[1]),
        pltpu.make_async_copy(up_ref.at[:, mine], wu.at[at], loc_sem.at[2]),
        pltpu.make_async_copy(down_ref.at[:, mine], wd.at[at], loc_sem.at[3]),
        pltpu.make_async_copy(tokens_ref.at[t], own, loc_sem.at[4]),
    ]
    for copy in local:
        copy.start()
    pl.semaphore_wait(barrier, n_fs + n_tp - 2)

    first = {}
    for k in range(1, group):
        first[k] = pltpu.make_async_remote_copy(
            normed_ref.at[t], xs.at[q, t], x_send.at[k], x_recv.at[k],
            device_id=(g * group + (q + k) % group, t), device_id_type=MESH,
        )
        first[k].start()
    moved = {}
    for a, (src, dst) in enumerate(((gate_ref, wg), (up_ref, wu), (down_ref, wd))):
        for dg in reversed(range(n_group)):
            for dq in range(group):
                if dg + dq > 0:
                    to_q = (q + dq) % group
                    part = pl.ds(pl.multiple_of(to_q * width, width), width)
                    moved[a, dg, dq] = pltpu.make_async_remote_copy(
                        src.at[:, part], dst.at[at],
                        w_send.at[a, dg * group + dq], w_recv.at[a, dg * group + dq],
                        device_id=(((g + dg) % n_group) * group + to_q, t), device_id_type=MESH,
                    )
                    moved[a, dg, dq].start()
    second = {}
    for k in range(1, group):
        first[k].wait_recv()
        of = (q + group - k) % group
        for m in range(1, n_tp):
            second[k, m] = pltpu.make_async_remote_copy(
                xs.at[of, t], xs.at[of, t], y_send.at[k, m], y_recv.at[k, m],
                device_id=(f, (t + m) % n_tp), device_id_type=MESH,
            )
            second[k, m].start()
    for copy in local:
        copy.wait()
    for copy in second.values():
        copy.wait_recv()
    for (a, dg, dq), copy in moved.items():
        if a < 2:
            copy.wait_recv()

    def hidden_block(b, carry):
        x = xs[b].reshape(rows, xs.shape[-1])
        gate = jnp.dot(x, wg[...], preferred_element_type=jnp.float32)
        up = jnp.dot(x, wu[...], preferred_element_type=jnp.float32)
        hid[b] = (gate / (1.0 + jnp.exp(-gate)) * up).astype(jnp.bfloat16)
        return carry

    lax.fori_loop(0, group, hidden_block, 0)

    def column(i):
        return ((g + i // SUB) % n_group) * SUB + i % SUB

    def reduction(i, s):
        bit = (rank // 2**s) % 2
        flip = 1 - 2 * bit
        if s < tp_bits:
            to = (f, t + flip * 2**s)
        else:
            to = (f + flip * 2 ** (s - tp_bits), t)
        return pltpu.make_async_remote_copy(
            held[s].at[i, :, 1 - bit], arrived[s].at[i], r_send.at[i, s], r_recv.at[i, s],
            device_id=to, device_id_type=MESH,
        )

    def down_chunk(i):
        if i % SUB == 0:
            dg = (n_group - i // SUB) % n_group
            for dq in range(group):
                if dg + dq > 0:
                    moved[2, dg, dq].wait_recv()
        cols = pl.ds(pl.multiple_of(column(i) * cw, cw), cw)

        def block(b, carry):
            part = lax.dot_general(
                hid[b], wd[cols, :], (((1,), (1,)), ((), ())), preferred_element_type=jnp.float32
            ).astype(jnp.bfloat16)
            held[0][i, pl.ds(b * (n_tp // 2), n_tp // 2)] = part.reshape(n_tp // 2, 2, rq, cw)
            return carry

        lax.fori_loop(0, group, block, 0)

    def add_stage(i, s):
        reduction(i, s).wait_recv()
        bit = (rank // 2**s) % 2
        if s == stages - 1:
            fin[i] = held[s][i, 0, bit].astype(jnp.float32) + arrived[s][i, 0].astype(jnp.float32)
            return

        def one(j, carry):
            total = held[s][i, j, bit].astype(jnp.float32) + arrived[s][i, j].astype(jnp.float32)
            held[s + 1][i, j // 2, j % 2] = total.astype(jnp.bfloat16)
            return carry

        lax.fori_loop(0, held[s].shape[1], one, 0)

    for step in range(chunks + stages):
        for s in reversed(range(stages)):
            i = step - s - 1
            if 0 <= i < chunks:
                add_stage(i, s)
                if s + 1 < stages:
                    reduction(i, s + 1).start()
        if step < chunks:
            down_chunk(step)
            reduction(step, 0).start()

    square = jnp.zeros((rq, 1), jnp.float32)
    for i in range(chunks):
        square += jnp.sum(fin[i] * fin[i], axis=-1, keepdims=True)
    scale = lax.rsqrt(square * (1.0 / (chunks * cw)) + epsilon)
    for i in range(chunks):
        cols = pl.ds(pl.multiple_of(column(i) * cw, cw), cw)
        out_ref[0, t, :, cols] = (
            own[:, cols].astype(jnp.float32) + fin[i] * scale * gain_ref[:, cols]
        ).astype(jnp.bfloat16)

    shared = []
    for s in reversed(range(tp_bits)):
        bit = (t // 2**s) % 2
        to = (f, t + (1 - 2 * bit) * 2**s)
        known = range(2 ** (tp_bits - 1 - s))
        batch = []
        for h in known:
            piece = out_ref.at[0, h * 2 ** (s + 1) + t % 2 ** (s + 1)]
            batch.append(pltpu.make_async_remote_copy(
                piece, piece, o_send.at[s, h], o_recv.at[s, h], device_id=to, device_id_type=MESH,
            ))
        for copy in batch:
            copy.start()
        for copy in batch:
            copy.wait_recv()
        shared += batch
    for copy in list(first.values()) + list(moved.values()) + list(second.values()) + shared:
        copy.wait_send()
    for i in range(chunks):
        for s in range(stages):
            reduction(i, s).wait_send()


def fused(n_fs, n_tp, group, tokens, norm_gain, gate_weight, up_weight, down_weight, branch_gain):
    rows, d = tokens.shape
    rq = rows // n_tp
    depth, hidden = gate_weight.shape
    width = hidden // group
    chunks = (n_fs // group) * SUB
    cw = d // chunks
    pieces = group * n_tp
    stages = log2(pieces)
    normed = normalize(tokens, norm_gain)
    bf16, dma = jnp.bfloat16, pltpu.SemaphoreType.DMA
    hbm = pl.BlockSpec(memory_space=pl.ANY)
    vmem = pl.BlockSpec(memory_space=pltpu.VMEM)
    out = pl.pallas_call(
        functools.partial(kernel, n_fs, n_tp, group),
        out_shape=jax.ShapeDtypeStruct((1, n_tp, rq, d), bf16),
        in_specs=[hbm] * 5 + [vmem],
        out_specs=vmem,
        scratch_shapes=[
            pltpu.VMEM((group, n_tp, rq, d), bf16),
            pltpu.VMEM((d, width), bf16),
            pltpu.VMEM((d, width), bf16),
            pltpu.VMEM((d, width), bf16),
            pltpu.VMEM((group, rows, width), bf16),
            pltpu.VMEM((rq, d), bf16),
            pltpu.VMEM((chunks, rq, cw), jnp.float32),
        ]
        + [pltpu.VMEM((chunks, pieces >> (s + 1), 2, rq, cw), bf16) for s in range(stages)]
        + [pltpu.VMEM((chunks, pieces >> (s + 1), rq, cw), bf16) for s in range(stages)]
        + [
            dma((5,)),
            dma((3, n_fs)), dma((3, n_fs)),
            dma((group,)), dma((group,)),
            dma((group, n_tp)), dma((group, n_tp)),
            dma((chunks, stages)), dma((chunks, stages)),
            dma((log2(n_tp), n_tp)), dma((log2(n_tp), n_tp)),
        ],
        compiler_params=pltpu.CompilerParams(
            collective_id=0, has_side_effects=True, vmem_limit_bytes=60 * 1024 * 1024
        ),
    )(
        tokens.reshape(n_tp, rq, d), normed.reshape(n_tp, rq, d),
        gate_weight, up_weight, down_weight.T, branch_gain.reshape(1, d),
    )
    return out.reshape(rows, d)


def solution(mesh):
    n_fs, n_tp = mesh.shape["fs"], mesh.shape["tp"]

    def per_device(*args):
        tokens, _, gate_weight = args[:3]
        rows, d = tokens.shape
        depth, hidden = gate_weight.shape
        group = 4
        fits = (
            n_fs % group == 0
            and n_tp & (n_tp - 1) == 0
            and n_tp > 1
            and rows % (16 * n_tp) == 0
            and depth % 16 == 0
            and hidden % (128 * group) == 0
            and d % (128 * SUB * max(n_fs // group, 1)) == 0
        )
        if fits:
            return fused(n_fs, n_tp, group, *args)
        return plain(*args)

    in_specs = (P("fs", None), P(), P("fs", "tp"), P("fs", "tp"), P("tp", "fs"), P())
    return jax.shard_map(
        per_device, mesh=mesh, in_specs=in_specs, out_specs=P("fs", None), check_vma=False
    )
```

```python
import functools

import jax
import jax.numpy as jnp
from jax import lax
from jax.experimental import pallas as pl
from jax.experimental.pallas import tpu as pltpu
from jax.sharding import PartitionSpec as P

MESH = pl.DeviceIdType.MESH
epsilon = 1e-06
SUB = 3


def complete(own_tokens, summed, branch_gain):
    branch_scale = lax.rsqrt(jnp.mean(summed * summed, axis=-1, keepdims=True) + epsilon)
    return (own_tokens.astype(jnp.float32) + summed * branch_scale * branch_gain).astype(
        jnp.bfloat16
    )


def normalize(tokens, norm_gain):
    widened = tokens.astype(jnp.float32)
    scale = lax.rsqrt(jnp.mean(widened * widened, axis=-1, keepdims=True) + epsilon)
    return (widened * scale * norm_gain).astype(jnp.bfloat16)


def plain(tokens, norm_gain, gate_weight, up_weight, down_weight, branch_gain):
    normed = normalize(tokens, norm_gain)
    gate_whole, up_whole = (
        lax.all_gather(gate_weight, "fs", axis=0, tiled=True),
        lax.all_gather(up_weight, "fs", axis=0, tiled=True),
    )
    gate_sum = jnp.dot(normed, gate_whole, preferred_element_type=jnp.float32)
    up_sum = jnp.dot(normed, up_whole, preferred_element_type=jnp.float32)
    hidden = (jax.nn.silu(gate_sum) * up_sum).astype(jnp.bfloat16)
    partial_value = jnp.dot(
        hidden,
        lax.all_gather(down_weight, "fs", axis=1, tiled=True),
        preferred_element_type=jnp.float32,
    )
    summed = lax.psum(partial_value.astype(jnp.bfloat16), "tp").astype(jnp.float32)
    return complete(tokens, summed, branch_gain)


def log2(n):
    return n.bit_length() - 1


def kernel(n_fs, n_tp, group, tokens_ref, gate_ref, up_ref, down_ref, gain_ref, out_ref, *scratch):
    n_group = n_fs // group
    stages = log2(group * n_tp)
    tp_bits = log2(n_tp)
    xs, xn, wg, wu, wd, hid = scratch[:6]
    held = scratch[6:6 + stages]
    arrived = scratch[6 + stages:6 + 2 * stages]
    (loc_sem, w_send, w_recv, x_send, x_recv, y_send, y_recv, r_send, r_recv, o_send, o_recv) = scratch[6 + 2 * stages:]
    f, t = lax.axis_index("fs"), lax.axis_index("tp")
    g, q = f // group, f % group
    rank = q * n_tp + t
    depth, width = gate_ref.shape[0], wg.shape[1]
    chunks, rq, cw = arrived[0].shape[0], *arrived[0].shape[2:]
    rows = n_tp * rq

    barrier = pltpu.get_barrier_semaphore()
    for k in range(1, n_fs):
        pl.semaphore_signal(barrier, inc=1, device_id=((f + k) % n_fs, t), device_id_type=MESH)
    for k in range(1, n_tp):
        pl.semaphore_signal(barrier, inc=1, device_id=(f, (t + k) % n_tp), device_id_type=MESH)

    at = pl.ds(pl.multiple_of(f * depth, depth), depth)
    mine = pl.ds(pl.multiple_of(q * width, width), width)
    local = [
        pltpu.make_async_copy(tokens_ref, xs.at[q], loc_sem.at[0]),
        pltpu.make_async_copy(gate_ref.at[:, mine], wg.at[at], loc_sem.at[1]),
        pltpu.make_async_copy(up_ref.at[:, mine], wu.at[at], loc_sem.at[2]),
        pltpu.make_async_copy(down_ref.at[:, mine], wd.at[at], loc_sem.at[3]),
    ]
    for copy in local:
        copy.start()
    pl.semaphore_wait(barrier, n_fs + n_tp - 2)

    first = {}
    for k in range(1, group):
        first[k] = pltpu.make_async_remote_copy(
            tokens_ref.at[t], xs.at[q, t], x_send.at[k], x_recv.at[k],
            device_id=(g * group + (q + k) % group, t), device_id_type=MESH,
        )
        first[k].start()
    moved = {}
    for a, (src, dst) in enumerate(((gate_ref, wg), (up_ref, wu), (down_ref, wd))):
        for dg in reversed(range(n_group)) if a < 2 else range(n_group):
            for dq in range(group):
                if dg + dq > 0:
                    to_q = (q + dq) % group
                    part = pl.ds(pl.multiple_of(to_q * width, width), width)
                    moved[a, dg, dq] = pltpu.make_async_remote_copy(
                        src.at[:, part], dst.at[at],
                        w_send.at[a, dg * group + dq], w_recv.at[a, dg * group + dq],
                        device_id=(((g + dg) % n_group) * group + to_q, t), device_id_type=MESH,
                    )
                    moved[a, dg, dq].start()
    def normalize_piece(block, piece):
        def strip(r, carry):
            at_rows = pl.ds(pl.multiple_of(r * 16, 16), 16)
            x = xs[block, piece, at_rows, :].astype(jnp.float32)
            scale = lax.rsqrt(jnp.mean(x * x, axis=-1, keepdims=True) + epsilon)
            xn[block, piece, at_rows, :] = (x * scale * gain_ref[...]).astype(jnp.bfloat16)
            return carry

        lax.fori_loop(0, rq // 16, strip, 0)

    for copy in local:
        copy.wait()
    for piece in range(n_tp):
        normalize_piece(q, piece)
    second = {}
    for k in range(1, group):
        first[k].wait_recv()
        of = (q + group - k) % group
        for m in range(1, n_tp):
            second[k, m] = pltpu.make_async_remote_copy(
                xs.at[of, t], xs.at[of, t], y_send.at[k, m], y_recv.at[k, m],
                device_id=(f, (t + m) % n_tp), device_id_type=MESH,
            )
            second[k, m].start()
        normalize_piece(of, t)
    for (k, m), copy in second.items():
        copy.wait_recv()
        normalize_piece((q + group - k) % group, (t + n_tp - m) % n_tp)
    for (a, dg, dq), copy in moved.items():
        if a < 2:
            copy.wait_recv()

    def hidden_block(b, carry):
        x = xn[b].reshape(rows, xn.shape[-1])
        gate = jnp.dot(x, wg[...], preferred_element_type=jnp.float32)
        up = jnp.dot(x, wu[...], preferred_element_type=jnp.float32)
        hid[b] = (gate / (1.0 + jnp.exp(-gate)) * up).astype(jnp.bfloat16)
        return carry

    lax.fori_loop(0, group, hidden_block, 0)

    def column(i):
        return ((g + i // SUB) % n_group) * SUB + i % SUB

    def order(i):
        rest = list(range(1, stages))
        turn = i % SUB % len(rest)
        return [0] + rest[turn:] + rest[:turn]

    def reduction(i, s):
        b = order(i)[s]
        bit = (rank // 2**b) % 2
        flip = 1 - 2 * bit
        if b < tp_bits:
            to = (f, t + flip * 2**b)
        else:
            to = (f + flip * 2 ** (b - tp_bits), t)
        return pltpu.make_async_remote_copy(
            held[s].at[i, :, 1 - bit], arrived[s].at[i], r_send.at[i, s], r_recv.at[i, s],
            device_id=to, device_id_type=MESH,
        )

    def columns(i):
        return pl.ds(pl.multiple_of(column(i) * cw, cw), cw)

    def down_chunk(i):
        def block(b, carry):
            part = lax.dot_general(
                hid[b], wd[columns(i), :], (((1,), (1,)), ((), ())),
                preferred_element_type=jnp.float32,
            ).astype(jnp.bfloat16)
            for piece in range(n_tp):
                owner = b * n_tp + piece
                place = sum((owner // 2**o) % 2 * 2**s for s, o in enumerate(order(i)))
                held[0][i, place // 2, place % 2] = part[piece * rq:(piece + 1) * rq]
            return carry

        lax.fori_loop(0, group, block, 0)

    def add_stage(i, s):
        reduction(i, s).wait_recv()
        bit = (rank // 2 ** order(i)[s]) % 2
        if s == stages - 1:
            total = held[s][i, 0, bit].astype(jnp.float32) + arrived[s][i, 0].astype(jnp.float32)
            out_ref[0, t, :, columns(i)] = total.astype(jnp.bfloat16)
            return

        def one(j, carry):
            total = held[s][i, j, bit].astype(jnp.float32) + arrived[s][i, j].astype(jnp.float32)
            held[s + 1][i, j // 2, j % 2] = total.astype(jnp.bfloat16)
            return carry

        lax.fori_loop(0, held[s].shape[1], one, 0)

    def sharing(i, s):
        bit = (t // 2**s) % 2
        copies = []
        for h in range(2 ** (tp_bits - 1 - s)):
            piece = out_ref.at[0, h * 2 ** (s + 1) + t % 2 ** (s + 1), :, columns(i)]
            copies.append(pltpu.make_async_remote_copy(
                piece, piece, o_send.at[i, s, h], o_recv.at[i, s, h],
                device_id=(f, t + (1 - 2 * bit) * 2**s), device_id_type=MESH,
            ))
        return copies

    for part in range(n_group):
        dg = (n_group - part) % n_group
        for dq in range(group):
            if dg + dq > 0:
                moved[2, dg, dq].wait_recv()
        here = range(part * SUB, (part + 1) * SUB)
        for i in here:
            down_chunk(i)
            reduction(i, 0).start()
        for s in range(stages):
            for i in here:
                add_stage(i, s)
                if s + 1 < stages:
                    reduction(i, s + 1).start()
                else:
                    for copy in sharing(i, tp_bits - 1):
                        copy.start()
        for s in reversed(range(tp_bits)):
            for i in here:
                for copy in sharing(i, s):
                    copy.wait_recv()
                if s > 0:
                    for copy in sharing(i, s - 1):
                        copy.start()

    for copy in list(first.values()) + list(moved.values()) + list(second.values()):
        copy.wait_send()
    for i in range(chunks):
        for s in range(stages):
            reduction(i, s).wait_send()
        for s in range(tp_bits):
            for copy in sharing(i, s):
                copy.wait_send()


def fused(n_fs, n_tp, group, tokens, norm_gain, gate_weight, up_weight, down_weight, branch_gain):
    rows, d = tokens.shape
    rq = rows // n_tp
    depth, hidden = gate_weight.shape
    width = hidden // group
    chunks = (n_fs // group) * SUB
    cw = d // chunks
    pieces = group * n_tp
    stages = log2(pieces)
    bf16, dma = jnp.bfloat16, pltpu.SemaphoreType.DMA
    hbm = pl.BlockSpec(memory_space=pl.ANY)
    vmem = pl.BlockSpec(memory_space=pltpu.VMEM)
    out = pl.pallas_call(
        functools.partial(kernel, n_fs, n_tp, group),
        out_shape=jax.ShapeDtypeStruct((1, n_tp, rq, d), bf16),
        in_specs=[hbm] * 4 + [vmem],
        out_specs=vmem,
        scratch_shapes=[
            pltpu.VMEM((group, n_tp, rq, d), bf16),
            pltpu.VMEM((group, n_tp, rq, d), bf16),
            pltpu.VMEM((d, width), bf16),
            pltpu.VMEM((d, width), bf16),
            pltpu.VMEM((d, width), bf16),
            pltpu.VMEM((group, rows, width), bf16),
        ]
        + [pltpu.VMEM((chunks, pieces >> (s + 1), 2, rq, cw), bf16) for s in range(stages)]
        + [pltpu.VMEM((chunks, pieces >> (s + 1), rq, cw), bf16) for s in range(stages)]
        + [
            dma((4,)),
            dma((3, n_fs)), dma((3, n_fs)),
            dma((group,)), dma((group,)),
            dma((group, n_tp)), dma((group, n_tp)),
            dma((chunks, stages)), dma((chunks, stages)),
            dma((chunks, log2(n_tp), n_tp)), dma((chunks, log2(n_tp), n_tp)),
        ],
        compiler_params=pltpu.CompilerParams(
            collective_id=0, has_side_effects=True, vmem_limit_bytes=60 * 1024 * 1024
        ),
    )(
        tokens.reshape(n_tp, rq, d), gate_weight, up_weight, down_weight.T, norm_gain.reshape(1, d),
    )
    return complete(tokens, out.reshape(rows, d).astype(jnp.float32), branch_gain)


def solution(mesh):
    n_fs, n_tp = mesh.shape["fs"], mesh.shape["tp"]

    def per_device(*args):
        tokens, _, gate_weight = args[:3]
        rows, d = tokens.shape
        depth, hidden = gate_weight.shape
        group = 4
        fits = (
            n_fs % group == 0
            and n_tp & (n_tp - 1) == 0
            and n_tp > 1
            and rows % (16 * n_tp) == 0
            and depth % 16 == 0
            and hidden % (128 * group) == 0
            and d % (128 * SUB * max(n_fs // group, 1)) == 0
        )
        if fits:
            return fused(n_fs, n_tp, group, *args)
        return plain(*args)

    in_specs = (P("fs", None), P(), P("fs", "tp"), P("fs", "tp"), P("tp", "fs"), P())
    return jax.shard_map(
        per_device, mesh=mesh, in_specs=in_specs, out_specs=P("fs", None), check_vma=False
    )
```

```python
import functools

import jax
import jax.numpy as jnp
from jax import lax
from jax.experimental import pallas as pl
from jax.experimental.pallas import tpu as pltpu
from jax.sharding import PartitionSpec as P

MESH = pl.DeviceIdType.MESH
epsilon = 1e-06
SUB = 3
LAG = 2


def complete(own_tokens, summed, branch_gain):
    branch_scale = lax.rsqrt(jnp.mean(summed * summed, axis=-1, keepdims=True) + epsilon)
    return (own_tokens.astype(jnp.float32) + summed * branch_scale * branch_gain).astype(
        jnp.bfloat16
    )


def normalize(tokens, norm_gain):
    widened = tokens.astype(jnp.float32)
    scale = lax.rsqrt(jnp.mean(widened * widened, axis=-1, keepdims=True) + epsilon)
    return (widened * scale * norm_gain).astype(jnp.bfloat16)


def plain(tokens, norm_gain, gate_weight, up_weight, down_weight, branch_gain):
    normed = normalize(tokens, norm_gain)
    gate_whole, up_whole = (
        lax.all_gather(gate_weight, "fs", axis=0, tiled=True),
        lax.all_gather(up_weight, "fs", axis=0, tiled=True),
    )
    gate_sum = jnp.dot(normed, gate_whole, preferred_element_type=jnp.float32)
    up_sum = jnp.dot(normed, up_whole, preferred_element_type=jnp.float32)
    hidden = (jax.nn.silu(gate_sum) * up_sum).astype(jnp.bfloat16)
    partial_value = jnp.dot(
        hidden,
        lax.all_gather(down_weight, "fs", axis=1, tiled=True),
        preferred_element_type=jnp.float32,
    )
    summed = lax.psum(partial_value.astype(jnp.bfloat16), "tp").astype(jnp.float32)
    return complete(tokens, summed, branch_gain)


def log2(n):
    return n.bit_length() - 1


def kernel(n_fs, n_tp, group, tokens_ref, gate_ref, up_ref, down_ref, gain_ref, out_ref, *scratch):
    n_group = n_fs // group
    stages = log2(group * n_tp)
    tp_bits = log2(n_tp)
    xs, xn, wg, wu, wd, hid, gated = scratch[:7]
    held = scratch[7:7 + stages]
    arrived = scratch[7 + stages:7 + 2 * stages]
    (loc_sem, w_send, w_recv, x_send, x_recv, y_send, y_recv, r_send, r_recv, o_send, o_recv) = scratch[7 + 2 * stages:]
    f, t = lax.axis_index("fs"), lax.axis_index("tp")
    g, q = f // group, f % group
    rank = q * n_tp + t
    depth, width = gate_ref.shape[0], wg.shape[1]
    chunks, rq, cw = arrived[0].shape[0], *arrived[0].shape[2:]
    rows = n_tp * rq

    barrier = pltpu.get_barrier_semaphore()
    for k in range(1, n_fs):
        pl.semaphore_signal(barrier, inc=1, device_id=((f + k) % n_fs, t), device_id_type=MESH)
    for k in range(1, n_tp):
        pl.semaphore_signal(barrier, inc=1, device_id=(f, (t + k) % n_tp), device_id_type=MESH)

    at = pl.ds(pl.multiple_of(f * depth, depth), depth)
    mine = pl.ds(pl.multiple_of(q * width, width), width)
    local = [
        pltpu.make_async_copy(tokens_ref, xs.at[q], loc_sem.at[0]),
        pltpu.make_async_copy(gate_ref.at[:, mine], wg.at[at], loc_sem.at[1]),
        pltpu.make_async_copy(up_ref.at[:, mine], wu.at[at], loc_sem.at[2]),
        pltpu.make_async_copy(down_ref.at[:, mine], wd.at[at], loc_sem.at[3]),
    ]
    for copy in local:
        copy.start()
    pl.semaphore_wait(barrier, n_fs + n_tp - 2)

    first = {}
    for k in range(1, group):
        first[k] = pltpu.make_async_remote_copy(
            tokens_ref.at[t], xs.at[q, t], x_send.at[k], x_recv.at[k],
            device_id=(g * group + (q + k) % group, t), device_id_type=MESH,
        )
        first[k].start()
    moved = {}
    for a, (src, dst) in enumerate(((gate_ref, wg), (up_ref, wu), (down_ref, wd))):
        for dg in reversed(range(n_group)) if a < 2 else range(n_group):
            for dq in range(group):
                if dg + dq > 0:
                    to_q = (q + dq) % group
                    part = pl.ds(pl.multiple_of(to_q * width, width), width)
                    moved[a, dg, dq] = pltpu.make_async_remote_copy(
                        src.at[:, part], dst.at[at],
                        w_send.at[a, dg * group + dq], w_recv.at[a, dg * group + dq],
                        device_id=(((g + dg) % n_group) * group + to_q, t), device_id_type=MESH,
                    )
                    moved[a, dg, dq].start()
    def normalize_piece(block, piece):
        def strip(r, carry):
            at_rows = pl.ds(pl.multiple_of(r * 16, 16), 16)
            x = xs[block, piece, at_rows, :].astype(jnp.float32)
            scale = lax.rsqrt(jnp.mean(x * x, axis=-1, keepdims=True) + epsilon)
            xn[block, piece, at_rows, :] = (x * scale * gain_ref[...]).astype(jnp.bfloat16)
            return carry

        lax.fori_loop(0, rq // 16, strip, 0)

    for copy in local:
        copy.wait()
    for piece in range(n_tp):
        normalize_piece(q, piece)
    def spread(k, s):
        of = (q + group - k) % group
        bit = (t // 2**s) % 2
        copies = []
        for h in range(2 ** (tp_bits - 1 - s)):
            piece = xs.at[of, h * 2 ** (s + 1) + t % 2 ** (s + 1)]
            copies.append(pltpu.make_async_remote_copy(
                piece, piece, y_send.at[k, s, h], y_recv.at[k, s, h],
                device_id=(f, t + (1 - 2 * bit) * 2**s), device_id_type=MESH,
            ))
        return copies

    for k in range(1, group):
        first[k].wait_recv()
        for copy in spread(k, tp_bits - 1):
            copy.start()
        normalize_piece((q + group - k) % group, t)
    for s in reversed(range(tp_bits)):
        other = (t % 2 ** (s + 1) + 2**s) % 2 ** (s + 1)
        for k in range(1, group):
            for copy in spread(k, s):
                copy.wait_recv()
            if s > 0:
                for copy in spread(k, s - 1):
                    copy.start()
            for h in range(2 ** (tp_bits - 1 - s)):
                normalize_piece((q + group - k) % group, h * 2 ** (s + 1) + other)

    def arrived_weight(a):
        for (b, _, _), copy in moved.items():
            if a == b:
                copy.wait_recv()

    def gate_block(b, carry):
        x = xn[b].reshape(rows, xn.shape[-1])
        gate = jnp.dot(x, wg[...], preferred_element_type=jnp.float32)
        gated[b] = gate / (1.0 + jnp.exp(-gate))
        return carry

    def up_block(b, carry):
        x = xn[b].reshape(rows, xn.shape[-1])
        up = jnp.dot(x, wu[...], preferred_element_type=jnp.float32)
        hid[b] = (gated[b] * up).astype(jnp.bfloat16)
        return carry

    arrived_weight(0)
    lax.fori_loop(0, group, gate_block, 0)
    arrived_weight(1)
    lax.fori_loop(0, group, up_block, 0)

    def column(i):
        return ((g + i // SUB) % n_group) * SUB + i % SUB

    def order(i):
        rest = list(range(1, stages))
        turn = i % SUB % len(rest)
        return [0] + rest[turn:] + rest[:turn]

    def reduction(i, s):
        b = order(i)[s]
        bit = (rank // 2**b) % 2
        flip = 1 - 2 * bit
        if b < tp_bits:
            to = (f, t + flip * 2**b)
        else:
            to = (f + flip * 2 ** (b - tp_bits), t)
        return pltpu.make_async_remote_copy(
            held[s].at[i, :, 1 - bit], arrived[s].at[i], r_send.at[i, s], r_recv.at[i, s],
            device_id=to, device_id_type=MESH,
        )

    def columns(i):
        return pl.ds(pl.multiple_of(column(i) * cw, cw), cw)

    def down_chunk(i):
        def block(b, carry):
            part = lax.dot_general(
                hid[b], wd[columns(i), :], (((1,), (1,)), ((), ())),
                preferred_element_type=jnp.float32,
            ).astype(jnp.bfloat16)
            for piece in range(n_tp):
                owner = b * n_tp + piece
                place = sum((owner // 2**o) % 2 * 2**s for s, o in enumerate(order(i)))
                held[0][i, place // 2, place % 2] = part[piece * rq:(piece + 1) * rq]
            return carry

        lax.fori_loop(0, group, block, 0)

    def add_stage(i, s):
        reduction(i, s).wait_recv()
        bit = (rank // 2 ** order(i)[s]) % 2
        if s == stages - 1:
            total = held[s][i, 0, bit].astype(jnp.float32) + arrived[s][i, 0].astype(jnp.float32)
            out_ref[0, t, :, columns(i)] = total.astype(jnp.bfloat16)
            return

        def one(j, carry):
            total = held[s][i, j, bit].astype(jnp.float32) + arrived[s][i, j].astype(jnp.float32)
            held[s + 1][i, j // 2, j % 2] = total.astype(jnp.bfloat16)
            return carry

        lax.fori_loop(0, held[s].shape[1], one, 0)

    def sharing(i, s):
        bit = (t // 2**s) % 2
        copies = []
        for h in range(2 ** (tp_bits - 1 - s)):
            piece = out_ref.at[0, h * 2 ** (s + 1) + t % 2 ** (s + 1), :, columns(i)]
            copies.append(pltpu.make_async_remote_copy(
                piece, piece, o_send.at[i, s, h], o_recv.at[i, s, h],
                device_id=(f, t + (1 - 2 * bit) * 2**s), device_id_type=MESH,
            ))
        return copies

    def begin(part):
        dg = (n_group - part) % n_group
        for dq in range(group):
            if dg + dq > 0:
                moved[2, dg, dq].wait_recv()
        for i in range(part * SUB, (part + 1) * SUB):
            down_chunk(i)
            reduction(i, 0).start()

    def advance(part, s):
        for i in range(part * SUB, (part + 1) * SUB):
            add_stage(i, s)
            if s + 1 < stages:
                reduction(i, s + 1).start()
            else:
                for copy in sharing(i, tp_bits - 1):
                    copy.start()

    def share(part, s):
        for i in range(part * SUB, (part + 1) * SUB):
            for copy in sharing(i, s):
                copy.wait_recv()
            if s > 0:
                for copy in sharing(i, s - 1):
                    copy.start()

    total_steps = 1 + stages + tp_bits
    for slot in range(total_steps + LAG * (n_group - 1)):
        for part in reversed(range(n_group)):
            step = slot - LAG * part
            if step == 0:
                begin(part)
            elif 1 <= step <= stages:
                advance(part, step - 1)
            elif stages < step < total_steps:
                share(part, tp_bits - 1 - (step - 1 - stages))

    for copy in list(first.values()) + list(moved.values()):
        copy.wait_send()
    for k in range(1, group):
        for s in range(tp_bits):
            for copy in spread(k, s):
                copy.wait_send()
    for i in range(chunks):
        for s in range(stages):
            reduction(i, s).wait_send()
        for s in range(tp_bits):
            for copy in sharing(i, s):
                copy.wait_send()


def fused(n_fs, n_tp, group, tokens, norm_gain, gate_weight, up_weight, down_weight, branch_gain):
    rows, d = tokens.shape
    rq = rows // n_tp
    depth, hidden = gate_weight.shape
    width = hidden // group
    chunks = (n_fs // group) * SUB
    cw = d // chunks
    pieces = group * n_tp
    stages = log2(pieces)
    bf16, dma = jnp.bfloat16, pltpu.SemaphoreType.DMA
    hbm = pl.BlockSpec(memory_space=pl.ANY)
    vmem = pl.BlockSpec(memory_space=pltpu.VMEM)
    out = pl.pallas_call(
        functools.partial(kernel, n_fs, n_tp, group),
        out_shape=jax.ShapeDtypeStruct((1, n_tp, rq, d), bf16),
        in_specs=[hbm] * 4 + [vmem],
        out_specs=vmem,
        scratch_shapes=[
            pltpu.VMEM((group, n_tp, rq, d), bf16),
            pltpu.VMEM((group, n_tp, rq, d), bf16),
            pltpu.VMEM((d, width), bf16),
            pltpu.VMEM((d, width), bf16),
            pltpu.VMEM((d, width), bf16),
            pltpu.VMEM((group, rows, width), bf16),
            pltpu.VMEM((group, rows, width), jnp.float32),
        ]
        + [pltpu.VMEM((chunks, pieces >> (s + 1), 2, rq, cw), bf16) for s in range(stages)]
        + [pltpu.VMEM((chunks, pieces >> (s + 1), rq, cw), bf16) for s in range(stages)]
        + [
            dma((4,)),
            dma((3, n_fs)), dma((3, n_fs)),
            dma((group,)), dma((group,)),
            dma((group, log2(n_tp), n_tp)), dma((group, log2(n_tp), n_tp)),
            dma((chunks, stages)), dma((chunks, stages)),
            dma((chunks, log2(n_tp), n_tp)), dma((chunks, log2(n_tp), n_tp)),
        ],
        compiler_params=pltpu.CompilerParams(
            collective_id=0, has_side_effects=True, vmem_limit_bytes=60 * 1024 * 1024
        ),
    )(
        tokens.reshape(n_tp, rq, d), gate_weight, up_weight, down_weight.T, norm_gain.reshape(1, d),
    )
    return complete(tokens, out.reshape(rows, d).astype(jnp.float32), branch_gain)


def solution(mesh):
    n_fs, n_tp = mesh.shape["fs"], mesh.shape["tp"]

    def per_device(*args):
        tokens, _, gate_weight = args[:3]
        rows, d = tokens.shape
        depth, hidden = gate_weight.shape
        group = 4
        fits = (
            n_fs % group == 0
            and n_tp & (n_tp - 1) == 0
            and n_tp > 1
            and rows % (16 * n_tp) == 0
            and depth % 16 == 0
            and hidden % (128 * group) == 0
            and d % (128 * SUB * max(n_fs // group, 1)) == 0
        )
        if fits:
            return fused(n_fs, n_tp, group, *args)
        return plain(*args)

    in_specs = (P("fs", None), P(), P("fs", "tp"), P("fs", "tp"), P("tp", "fs"), P())
    return jax.shard_map(
        per_device, mesh=mesh, in_specs=in_specs, out_specs=P("fs", None), check_vma=False
    )
```
